32 devices in a mesh: ep: 8 (over z, x), tp: 4 (over y, core).
Axes of the slice: x: 2, y: 2, z: 4, core: 2. Of those that a mesh axis runs over, the one named last changes fastest.
Arguments:
- tokens: bfloat16 [1024, 4096], P('ep', 'tp'), may hold values from -6 to 6
- cotangent: bfloat16 [1024, 4096], P('ep', 'tp'), may hold values from -6 to 6
- routes: int32 [1024, 2], P('ep'), may hold values from 0 to 7, all different within a row; in each aligned block of 128 rows (0 to 127, 128 to 255, ...) at most 48 rows name the same one
- gate_weight: float32 [1024, 2], P('ep'), may hold values from 0.1 to 2.5
- w_gate: bfloat16 [8, 1024, 4096], P('ep', 'tp'), may hold values from -0.09375 to 0.09375
- w_up: bfloat16 [8, 1024, 4096], P('ep', 'tp'), may hold values from -0.09375 to 0.09375
- w_down: bfloat16 [8, 1024, 4096], P('ep', 'tp'), may hold values from -0.1875 to 0.1875
- shared_hidden: bfloat16 [1024, 1024], P('ep'), may hold values from -4 to 4
Outputs:
- tokens_grad: bfloat16 [1024, 4096], P('ep', 'tp')
- gate_grad: float32 [1024, 2], P('ep')
- w_gate_grad: float32 [8, 1024, 4096], P('ep', 'tp')
- w_up_grad: float32 [8, 1024, 4096], P('ep', 'tp')
- w_down_grad: float32 [8, 1024, 4096], P('ep', 'tp')
- shared_grad: float32 [1024, 4096], P('ep', 'tp')
The draws below stay inside these ranges and needn't reach their ends.
Inputs may be any that keep to these rules, and one draw needn't show every extreme that they name: `routes`: each row names 2 different experts. Among the rows of one index of ep (aligned blocks of 128 rows) no expert is named more than 48 times, and in every draw some expert is named exactly 48 times in some block.
All inputs are finite; a program needn't handle non-finite values.
Results may differ from the reference program's by a relative error of at most 0.022.
Values may be sent and summed in bfloat16 or wider, within the bound.
A program may use at most 64 MiB of HBM per device.

```python
import math
import jax
import jax.numpy as jnp
import numpy as np
from jax import lax

D = 4096
HIDDEN_SIZE = 1024
SHARED_HIDDEN = 1024
TOP_K = 2
TOK_DEV = 128
EXPERTS = 8
CAP = 48
TOKENS = 1024
N_EP = 8
N_TP = 4


def with_spikes(drawn, rng, source, target, parts, factor):
    def block_of(position):
        return (jnp.arange(drawn.shape[position]) // (drawn.shape[position] // parts)).reshape((-1,) + (1,) * (drawn.ndim - 1 - position))

    near = jax.random.permutation(rng, parts)[block_of(target)]
    second = (block_of(target) + parts // 2) % parts
    return jnp.where((block_of(source) == near) | (block_of(source) == second), factor * drawn, drawn)


def levels(rng, shape, pieces, low, largest):
    def one(axis_at, shards_of):
        heights = jax.random.uniform(jax.random.fold_in(jax.random.fold_in(rng, 6), axis_at), (shards_of,), jnp.float32, low / len(pieces), largest / len(pieces))
        return jnp.repeat(jnp.exp(heights), shape[axis_at] // shards_of).reshape((-1,) + (1,) * (len(shape) - axis_at - 1))

    level = one(*pieces[0])
    for cut in pieces[1:]:
        level = level * one(*cut)
    return level


def deal_out(rng, own, number, rows, count, top, bound, lean):
    ranking = jax.random.permutation(rng, count)
    packed, common = portions_of(count, rows * top, bound, lean, True), portions_of(count, rows * top, bound, lean, False)
    places = jnp.arange(count)

    def named(tallies, turn):
        used = int((tallies > 0).sum())
        fixed = max(1, used // 4)
        moved = fixed + (places - fixed + turn * (used - fixed)) % max(1, count - fixed)
        return jnp.zeros((count,), jnp.int32).at[ranking[jnp.where(places < fixed, places, moved)]].set(jnp.asarray(tallies, jnp.int32))

    tallies = jnp.where(number % 4 == 0, named(packed, number // 4), named(common, number - number // 4 - 1))
    mixed = jax.random.permutation(jax.random.fold_in(own, 3), count)
    giver, receiver = mixed[0:count // 2 * 2:2], mixed[1:count // 2 * 2:2]
    room = jnp.minimum(tallies[giver] - 1, bound - tallies[receiver]) // 2
    room = jnp.where((giver == ranking[0]) | (receiver == ranking[0]) | (tallies[receiver] == 0), 0, jnp.maximum(room, 0))
    moved = jax.random.randint(jax.random.fold_in(own, 4), (count // 2,), 0, 1 << 20) % (room + 1)
    tallies = tallies.at[giver].add(-moved).at[receiver].add(moved)
    items = jnp.searchsorted(jnp.cumsum(tallies), jnp.arange(rows * top), side="right").astype(jnp.int32)
    table = items.reshape(top, rows).T
    table = table[jax.random.permutation(jax.random.fold_in(own, 1), rows)]
    turn = jax.random.randint(jax.random.fold_in(own, 2), (rows, 1), 0, top)
    return jnp.take_along_axis(table, (jnp.arange(top)[None, :] + turn) % top, axis=1)


def portions_of(count, total, limit, slope, full):
    portions = [(1 << 20) // math.isqrt(grade ** slope) + 1 for grade in range(1, count + 1)]
    largest = limit if full else min(limit, max(-(-total // count), total * portions[0] // sum(portions)))
    least = 1 if total - largest >= count - 1 else 0
    holding, surplus = [largest] + [least] * (count - 1), total - largest - least * (count - 1)
    while surplus > 0:
        movable = [i for i in range(1, count) if holding[i] < largest] or [i for i in range(1, count) if holding[i] < limit]
        whole, left = sum([portions[i] for i in movable]), surplus
        for i in movable:
            extra = min(limit - holding[i], max(1, left * portions[i] // whole), surplus)
            holding[i] = holding[i] + extra
            surplus = surplus - extra
    return np.array(holding)


def centred(key, dims, spread, bound, split=(), kind=jnp.bfloat16):
    drawn = spread * jax.random.normal(key, dims, jnp.float32)
    if split:
        drawn = drawn * levels(key, dims, split, -0.22, 0.18)
    return jnp.clip(drawn, -bound, bound).astype(kind)


def bell_draw_with(stream_key, extent, spread, most, cuts, heavy, kind=jnp.bfloat16):
    drawn = spread * jax.random.normal(stream_key, extent, jnp.float32)
    if cuts:
        drawn = drawn * levels(stream_key, extent, cuts, -0.22, 0.18)
    return jnp.clip(with_spikes(drawn, jax.random.fold_in(stream_key, 3), *heavy), -most, most).astype(kind)


def setup_inputs(seed: int = 0) -> dict:
    key_list = jax.random.split(jax.random.key(seed), 9)
    tokens = centred(key_list[0], (TOKENS, D), 1.0, 6.0, ((0, 8), (1, 4)))
    cotangent = centred(key_list[1], (TOKENS, D), 1.0, 6.0, ((0, 8), (1, 4)))
    routes_keys = jax.random.split(jax.random.fold_in(key_list[2], 1), TOKENS // TOK_DEV)
    routes_turns = jax.random.permutation(jax.random.fold_in(key_list[2], 3), TOKENS // TOK_DEV)
    routes = jax.vmap(lambda own, number: deal_out(jax.random.fold_in(key_list[2], 2), own, number, TOK_DEV, EXPERTS, TOP_K, CAP, 2))(routes_keys, routes_turns).reshape((TOKENS, TOP_K))
    gate_weight = jnp.clip(jnp.exp(math.log(2.5) - 3.218876 * jax.random.uniform(key_list[3], (TOKENS, TOP_K), jnp.float32) ** levels(key_list[3], (TOKENS, TOP_K), ((0, 8),), -0.2, 0.2)), 0.1, 2.5)
    w_gate = centred(key_list[4], (EXPERTS, HIDDEN_SIZE, D), D ** -0.5, 0.09375, ((0, 8), (1, 4)))
    w_up = centred(key_list[5], (EXPERTS, HIDDEN_SIZE, D), D ** -0.5, 0.09375, ((0, 8), (1, 4)))
    w_down = centred(key_list[6], (EXPERTS, HIDDEN_SIZE, D), HIDDEN_SIZE ** -0.5, 0.1875, ((0, 8), (1, 4)))
    shared_hidden = bell_draw_with(key_list[7], (TOKENS, SHARED_HIDDEN), 0.5, 4.0, ((0, 8),), (0, 1, 8, 2.0))
    return {"tokens": tokens, "cotangent": cotangent, "routes": routes, "gate_weight": gate_weight, "w_gate": w_gate, "w_up": w_up, "w_down": w_down, "shared_hidden": shared_hidden}


def slot_positions(device_routes):
    flat_routes = device_routes.reshape(-1)
    onehot = (flat_routes[:, None] == jnp.arange(EXPERTS, dtype=jnp.int32)[None, :]).astype(jnp.int32)
    earlier = jnp.cumsum(onehot, axis=0) - onehot
    return flat_routes, jnp.sum(earlier * onehot, axis=1).astype(jnp.int32)


def reference(tokens, cotangent, routes, gate_weight, w_gate, w_up, w_down, shared_hidden):
    assigned = TOK_DEV * TOP_K
    flat_routes, positions = jax.vmap(slot_positions)(routes.reshape(N_EP, assigned))
    sources = jnp.broadcast_to(jnp.arange(N_EP, dtype=jnp.int32)[:, None], (N_EP, assigned))
    token_ids = sources * TOK_DEV + jnp.arange(assigned, dtype=jnp.int32)[None, :] // TOP_K
    slot_table = jnp.full((EXPERTS, N_EP, CAP), TOKENS, jnp.int32).at[flat_routes, sources, positions].set(token_ids)
    weight_table = jnp.zeros((EXPERTS, N_EP, CAP), jnp.float32).at[flat_routes, sources, positions].set(
        gate_weight.reshape(N_EP, assigned))
    padded_tokens = jnp.concatenate([tokens, jnp.zeros((1, D), jnp.bfloat16)], 0)
    padded_cotan = jnp.concatenate([cotangent, jnp.zeros((1, D), jnp.bfloat16)], 0)
    groups = HIDDEN_SIZE // N_TP
    contract_last = (((1,), (1,)), ((), ()))

    def expert_fn(inputs):
        table_rows, weight_rows, gate_mat, up_mat, down_mat = inputs
        rows_x = padded_tokens[table_rows.reshape(-1)]
        rows_g = padded_cotan[table_rows.reshape(-1)]
        weight_col = weight_rows.reshape(-1, 1)
        pre_gate = lax.dot_general(rows_x, gate_mat, contract_last, preferred_element_type=jnp.float32)
        pre_up = lax.dot_general(rows_x, up_mat, contract_last, preferred_element_type=jnp.float32)
        sigmoid_gate = jax.nn.sigmoid(pre_gate)
        silu_gate = pre_gate * sigmoid_gate
        hidden = (silu_gate * pre_up).astype(jnp.bfloat16)
        back_hidden = lax.dot_general(rows_g, down_mat, contract_last, preferred_element_type=jnp.float32)
        gate_part = jnp.sum(hidden.astype(jnp.float32) * back_hidden, axis=1)
        scaled = weight_col * back_hidden
        grad_pre_gate = (scaled * pre_up * sigmoid_gate * (1.0 + pre_gate * (1.0 - sigmoid_gate))).astype(jnp.bfloat16)
        grad_pre_up = (scaled * silu_gate).astype(jnp.bfloat16)
        weighted_cotan = (weight_col * rows_g.astype(jnp.float32)).astype(jnp.bfloat16)
        grad_down = jnp.dot(hidden.T, weighted_cotan, preferred_element_type=jnp.float32)
        grad_gate = jnp.dot(grad_pre_gate.T, rows_x, preferred_element_type=jnp.float32)
        grad_up = jnp.dot(grad_pre_up.T, rows_x, preferred_element_type=jnp.float32)
        row_total = rows_x.shape[0]
        partial_value = jnp.einsum('rnh,nhd->nrd', grad_pre_gate.astype(jnp.float32).reshape(row_total, N_TP, groups),
                             gate_mat.astype(jnp.float32).reshape(N_TP, groups, D))
        partial_value = partial_value + jnp.einsum('rnh,nhd->nrd', grad_pre_up.astype(jnp.float32).reshape(row_total, N_TP, groups),
                                       up_mat.astype(jnp.float32).reshape(N_TP, groups, D))
        rounded = lax.optimization_barrier(partial_value.astype(jnp.bfloat16)).astype(jnp.float32)
        row_grad = jnp.sum(rounded, axis=0).astype(jnp.bfloat16)
        return row_grad.reshape(N_EP, CAP, D), gate_part.reshape(N_EP, CAP), grad_gate, grad_up, grad_down

    row_grads, gate_parts, w_gate_grad, w_up_grad, w_down_grad = lax.map(
        expert_fn, (slot_table, weight_table, w_gate, w_up, w_down))
    picked = row_grads[flat_routes, sources, positions].astype(jnp.float32)
    tokens_grad = jnp.sum(picked.reshape(TOKENS, TOP_K, D), axis=1).astype(jnp.bfloat16)
    gate_grad = gate_parts[flat_routes, sources, positions].reshape(TOKENS, TOP_K)
    shared_grad = jnp.dot(shared_hidden.T, cotangent, preferred_element_type=jnp.float32)
    return (tokens_grad, gate_grad, w_gate_grad, w_up_grad, w_down_grad, shared_grad)
```

```python
import functools

import jax
import jax.numpy as jnp
from jax import lax
from jax.experimental import pallas as pl
from jax.experimental.pallas import tpu as pltpu
from jax.sharding import PartitionSpec as P

MESH = pl.DeviceIdType.MESH
BF16 = jnp.bfloat16
F32 = jnp.float32


def dispatch_kernel(
    dims,
    tok_ref,
    meta_ref,
    cot_ref,
    sh_ref,
    xfull,
    gfull,
    meta_out,
    cot_all,
    sh_out,
    local_sem,
    meta_send,
    meta_recv,
    tok_send,
    tok_recv,
    sh_send,
    sh_recv,
    cot_up,
    cot_down,
    cot_side,
    cot_recv,
    y_send,
    y_recv,
    sib_send,
    sib_recv,
):
    E, T, X, C, F, N = dims
    Y = T // 2
    NZ = E // X
    me = lax.axis_index("ep")
    tp = lax.axis_index("tp")
    y = tp // 2
    c = tp % 2
    sib = y * 2 + (1 - c)
    z = me // X
    x = me % X
    full = (xfull, gfull)

    barrier = pltpu.get_barrier_semaphore()

    def greet(d, _):
        pl.semaphore_signal(
            barrier, inc=1, device_id=((me + d) % E, tp), device_id_type=MESH
        )
        return 0

    lax.fori_loop(1, E, greet, 0)
    for dy in range(1, Y):
        pl.semaphore_signal(
            barrier, inc=1, device_id=(me, ((y + dy) % Y) * 2 + c), device_id_type=MESH
        )
    pl.semaphore_signal(barrier, inc=1, device_id=(me, sib), device_id_type=MESH)
    pl.semaphore_wait(barrier, (E - 1) + (Y - 1) + 1)

    def rows_of(s):
        return pl.ds(pl.multiple_of(s * C, 16), C)

    def cols_of(t):
        return pl.ds(pl.multiple_of(t * F, 128), F)

    def lanes_of(s):
        return pl.ds(pl.multiple_of(s * N, 128), N)

    def remote(src, dst, ss, rs, dev):
        return pltpu.make_async_remote_copy(
            src_ref=src,
            dst_ref=dst,
            send_sem=ss,
            recv_sem=rs,
            device_id=dev,
            device_id_type=MESH,
        )

    def meta_copy(dst):
        return remote(
            meta_ref.at[dst], meta_out.at[me], meta_send.at[dst], meta_recv.at[me], (dst, tp)
        )

    def tok_copy(dst):
        return remote(
            tok_ref.at[dst],
            xfull.at[rows_of(me), cols_of(tp)],
            tok_send.at[dst],
            tok_recv.at[me],
            (dst, tp),
        )

    def sh_copy(dst):
        return remote(
            sh_ref.at[dst], sh_out.at[:, lanes_of(me)], sh_send.at[dst], sh_recv.at[me], (dst, tp)
        )

    def cot_copy(s, sems, dst):
        return remote(cot_all.at[s], cot_all.at[s], sems.at[s], cot_recv.at[s], (dst, tp))

    locals_ = (
        pltpu.make_async_copy(cot_ref, cot_all.at[me], local_sem.at[0]),
        pltpu.make_async_copy(
            tok_ref.at[me], xfull.at[rows_of(me), cols_of(tp)], local_sem.at[1]
        ),
        pltpu.make_async_copy(meta_ref.at[me], meta_out.at[me], local_sem.at[2]),
        pltpu.make_async_copy(sh_ref.at[me], sh_out.at[:, lanes_of(me)], local_sem.at[3]),
    )
    for cp in locals_:
        cp.start()
    for cp in locals_:
        cp.wait()

    def each_source(fn, first=0):
        def step(i, _):
            k = i // X
            dz = ((k + 1) // 2) * (1 - 2 * (k % 2))
            zs = z + dz
            dx = i % X

            @pl.when((zs >= 0) & (zs < NZ))
            def _():
                fn(i, dz, dx, zs * X + (x + dx) % X)

            return 0

        lax.fori_loop(first, (2 * NZ - 1) * X, step, 0)

    def spread_cot(dz, s, act):
        @pl.when((dz <= 0) & (z + 1 < NZ))
        def _():
            act(cot_copy(s, cot_up, me + X))

        @pl.when((dz >= 0) & (z >= 1))
        def _():
            act(cot_copy(s, cot_down, me - X))

        for d in range(1, X):
            act(cot_copy(s, cot_side.at[d - 1], z * X + (x + d) % X))

    def start(cp):
        cp.start()

    def wait_send(cp):
        cp.wait_send()

    spread_cot(me * 0, me, start)

    def send_small(i, dz, dx, s):
        meta_copy(s).start()

    def send_rows(i, dz, dx, s):
        tok_copy(s).start()

    def send_shared(i, dz, dx, s):
        sh_copy(s).start()

    each_source(send_small, 1)
    each_source(send_rows, 1)
    each_source(send_shared, 1)

    def y_copy(a, s, dy):
        part = full[a].at[rows_of(s), cols_of(tp)]
        return remote(
            part,
            part,
            y_send.at[a, dy - 1],
            y_recv.at[a, dy - 1, s],
            (me, ((y + dy) % Y) * 2 + c),
        )

    def sib_copy(a, s, dy):
        part = full[a].at[rows_of(s), cols_of(((y + Y - dy) % Y) * 2 + c)]
        return remote(part, part, sib_send.at[a, dy], sib_recv.at[a, dy], (me, sib))

    def take(i, dz, dx, s):
        @pl.when(s != me)
        def _():
            remote(
                cot_all.at[s], cot_all.at[s], cot_up.at[s], cot_recv.at[s], (me, tp)
            ).wait_recv()

            @pl.when(dx == 0)
            def _():
                spread_cot(dz, s, start)

            remote(
                meta_ref.at[s], meta_out.at[s], meta_send.at[s], meta_recv.at[s], (me, tp)
            ).wait_recv()

        picked = jnp.dot(
            meta_out[s, :, :N], cot_all[s], preferred_element_type=F32
        ).astype(BF16)
        gfull[rows_of(s), cols_of(tp)] = picked

        @pl.when(s != me)
        def _():
            remote(
                tok_ref.at[s],
                xfull.at[rows_of(s), cols_of(tp)],
                tok_send.at[s],
                tok_recv.at[s],
                (me, tp),
            ).wait_recv()

        for a in (0, 1):
            for dy in range(1, Y):
                y_copy(a, s, dy).start()
            sib_copy(a, s, 0).start()

    def relay(i, dz, dx, s):
        for a in (0, 1):
            for dy in range(1, Y):
                part = full[a].at[rows_of(s), cols_of(((y + Y - dy) % Y) * 2 + c)]
                remote(
                    part, part, y_send.at[a, dy - 1], y_recv.at[a, dy - 1, s], (me, tp)
                ).wait_recv()
                sib_copy(a, s, dy).start()

    def guarded(fn, j):
        k = j // X
        dz = ((k + 1) // 2) * (1 - 2 * (k % 2))
        zs = z + dz
        dx = j % X

        @pl.when((j >= 0) & (zs >= 0) & (zs < NZ))
        def _():
            fn(j, dz, dx, zs * X + (x + dx) % X)

    total = (2 * NZ - 1) * X

    def main(i, _):
        guarded(take, i)
        guarded(relay, i - X)
        return 0

    lax.fori_loop(0, total, main, 0)
    for j in range(total - X, total):
        guarded(relay, jnp.int32(j))

    def finish(i, dz, dx, s):
        @pl.when(s != me)
        def _():
            meta_copy(s).wait_send()
            tok_copy(s).wait_send()
            sh_copy(s).wait_send()
            remote(
                sh_ref.at[s], sh_out.at[:, lanes_of(s)], sh_send.at[s], sh_recv.at[s], (me, tp)
            ).wait_recv()

        @pl.when(dx == 0)
        def _():
            spread_cot(dz, s, wait_send)

    each_source(finish)
    for a in (0, 1):
        mine = full[a].at[:, cols_of(tp)]
        for dy in range(1, Y):
            remote(mine, mine, y_send.at[a, dy - 1], y_send.at[a, dy - 1], (me, sib)).wait_send()
        for dy in range(Y):
            other = full[a].at[:, cols_of(((y + Y - dy) % Y) * 2 + 1 - c)]
            cp = remote(other, other, sib_send.at[a, dy], sib_recv.at[a, dy], (me, sib))
            cp.wait_send()
            cp.wait_recv()


def dispatch(E, T, C, F, N, rows, meta, cotangent, shared):
    X = 2 if E % 2 == 0 else 1
    Y = T // 2
    S = shared.shape[1]
    M = meta.shape[2]
    dma = pltpu.SemaphoreType.DMA
    vmem = pl.BlockSpec(memory_space=pltpu.VMEM)
    return pl.pallas_call(
        functools.partial(dispatch_kernel, (E, T, X, C, F, N)),
        out_shape=(
            jax.ShapeDtypeStruct((E * C, T * F), BF16),
            jax.ShapeDtypeStruct((E * C, T * F), BF16),
            jax.ShapeDtypeStruct((E, C, M), BF16),
            jax.ShapeDtypeStruct((E, N, F), BF16),
            jax.ShapeDtypeStruct((S, E * N), BF16),
        ),
        in_specs=[vmem] * 4,
        out_specs=(vmem,) * 5,
        scratch_shapes=[
            dma((4,)),
            dma((E,)),
            dma((E,)),
            dma((E,)),
            dma((E,)),
            dma((E,)),
            dma((E,)),
            dma((E,)),
            dma((E,)),
            dma((max(X - 1, 1), E)),
            dma((E,)),
            dma((2, max(Y - 1, 1))),
            dma((2, max(Y - 1, 1), E)),
            dma((2, Y)),
            dma((2, Y)),
        ],
        compiler_params=pltpu.CompilerParams(
            collective_id=0, has_side_effects=True, vmem_limit_bytes=48 * 1024 * 1024
        ),
        name="dispatch",
    )(rows, meta, cotangent, shared)


def shards(tokens, cotangent, routes, gate_weight, w_gate, w_up, w_down, shared_hidden):
    tok_count, top_count = routes.shape
    E = lax.axis_size("ep")
    T = lax.axis_size("tp")
    F = tokens.shape[1]
    capacity = 3 * tok_count * top_count // (2 * E)
    C = -(-capacity // 16) * 16
    R = E * C
    flat_routes = routes.reshape(-1)
    onehot = (flat_routes[:, None] == jnp.arange(E, dtype=jnp.int32)[None, :]).astype(F32)
    count = tok_count * top_count
    before = (
        jnp.arange(count, dtype=jnp.int32)[:, None] > jnp.arange(count, dtype=jnp.int32)[None, :]
    ).astype(BF16)
    earlier = jnp.dot(before, onehot.astype(BF16), preferred_element_type=F32)
    positions = jnp.sum(earlier * onehot, axis=1).astype(jnp.int32)
    slots = (flat_routes * C + positions).reshape(tok_count, top_count)
    lines = jnp.arange(R, dtype=jnp.int32)[:, None]
    masks = [slots[:, k][None, :] == lines for k in range(top_count)]
    select = functools.reduce(jnp.logical_or, masks).astype(BF16)
    weight = sum(
        jnp.sum(jnp.where(m, gate_weight[:, k][None, :], 0.0), axis=1)
        for k, m in enumerate(masks)
    )
    high = lax.reduce_precision(weight, 8, 7)
    low = weight - high
    tail = jnp.arange(128, dtype=jnp.int32)[None, :]
    extra = jnp.where(
        tail == 0, high[:, None], jnp.where(tail == 1, low[:, None], 0.0)
    ).astype(BF16)
    meta = jnp.concatenate([select, extra], axis=1).reshape(E, C, tok_count + 128)
    rows = jnp.dot(select, tokens, preferred_element_type=F32).astype(BF16).reshape(E, C, F)
    shared = shared_hidden.T.reshape(E, shared_hidden.shape[1] // E, tok_count)

    rows_x, rows_g, meta_got, cot_all, shared_got = dispatch(
        E, T, C, F, tok_count, rows, meta, cotangent, shared
    )
    got = meta_got.reshape(R, tok_count + 128)
    weight_col = got[:, tok_count : tok_count + 1].astype(F32) + got[
        :, tok_count + 1 : tok_count + 2
    ].astype(F32)
    contract_last = (((1,), (1,)), ((), ()))
    gate_mat = w_gate[0]
    up_mat = w_up[0]
    down_mat = w_down[0]
    pre_gate = lax.dot_general(rows_x, gate_mat, contract_last, preferred_element_type=F32)
    pre_up = lax.dot_general(rows_x, up_mat, contract_last, preferred_element_type=F32)
    sigmoid_gate = jax.nn.sigmoid(pre_gate)
    silu_gate = pre_gate * sigmoid_gate
    hidden = (silu_gate * pre_up).astype(BF16)
    back_hidden = lax.dot_general(rows_g, down_mat, contract_last, preferred_element_type=F32)
    gate_part = jnp.sum(hidden.astype(F32) * back_hidden, axis=1)
    scaled = weight_col * back_hidden
    grad_pre_gate = (
        scaled * pre_up * sigmoid_gate * (1.0 + pre_gate * (1.0 - sigmoid_gate))
    ).astype(BF16)
    grad_pre_up = (scaled * silu_gate).astype(BF16)
    weighted_cotan = (weight_col * rows_g.astype(F32)).astype(BF16)
    grad_down = jnp.dot(hidden.T, weighted_cotan, preferred_element_type=F32)
    grad_gate = jnp.dot(grad_pre_gate.T, rows_x, preferred_element_type=F32)
    grad_up = jnp.dot(grad_pre_up.T, rows_x, preferred_element_type=F32)
    partial_value = jnp.dot(grad_pre_gate, gate_mat, preferred_element_type=F32)
    partial_value = partial_value + jnp.dot(grad_pre_up, up_mat, preferred_element_type=F32)
    shared_grad = jnp.dot(
        shared_got, cot_all.reshape(E * tok_count, F), preferred_element_type=F32
    )
    row_share = lax.psum_scatter(
        partial_value.astype(BF16).reshape(E, C, T * F), "tp", scatter_dimension=2, tiled=True
    )
    gate_total = lax.psum(gate_part.reshape(E, C), "tp")
    back_rows = lax.all_to_all(row_share, "ep", split_axis=0, concat_axis=0, tiled=True)
    back_gate = lax.all_to_all(
        gate_total.astype(BF16), "ep", split_axis=0, concat_axis=0, tiled=True
    ).astype(F32)
    tokens_grad = lax.dot_general(
        select, back_rows.reshape(R, F), (((0,), (0,)), ((), ())), preferred_element_type=F32
    ).astype(BF16)
    gate_grad = jnp.stack(
        [jnp.sum(jnp.where(m, back_gate.reshape(R, 1), 0.0), axis=0) for m in masks], axis=1
    )
    return (tokens_grad, gate_grad, grad_gate[None], grad_up[None], grad_down[None], shared_grad)


def solution(mesh):
    placed = (
        P("ep", "tp"),
        P("ep", "tp"),
        P("ep", None),
        P("ep", None),
        P("ep", "tp", None),
        P("ep", "tp", None),
        P("ep", "tp", None),
        P("ep", None),
    )
    return jax.shard_map(
        shards,
        mesh=mesh,
        in_specs=placed,
        out_specs=(
            P("ep", "tp"),
            P("ep", None),
            P("ep", "tp", None),
            P("ep", "tp", None),
            P("ep", "tp", None),
            P("ep", "tp"),
        ),
        check_vma=False,
    )
```

```python
import functools

import jax
import jax.numpy as jnp
from jax import lax
from jax.experimental import pallas as pl
from jax.experimental.pallas import tpu as pltpu
from jax.sharding import PartitionSpec as P

MESH = pl.DeviceIdType.MESH
BF16 = jnp.bfloat16
F32 = jnp.float32


def dispatch_kernel(
    dims,
    tok_ref,
    meta_ref,
    cot_ref,
    sh_ref,
    xfull,
    gfull,
    meta_out,
    cot_all,
    sh_out,
    local_sem,
    meta_send,
    meta_recv,
    tok_send,
    tok_recv,
    sh_send,
    sh_recv,
    cot_up,
    cot_down,
    cot_side,
    cot_recv,
    y_send,
    y_recv,
    sib_send,
    sib_recv,
):
    E, T, X, C, F, N = dims
    Y = T // 2
    NZ = E // X
    me = lax.axis_index("ep")
    tp = lax.axis_index("tp")
    y = tp // 2
    c = tp % 2
    sib = y * 2 + (1 - c)
    z = me // X
    x = me % X
    full = (xfull, gfull)

    barrier = pltpu.get_barrier_semaphore()

    def greet(d, _):
        pl.semaphore_signal(
            barrier, inc=1, device_id=((me + d) % E, tp), device_id_type=MESH
        )
        return 0

    lax.fori_loop(1, E, greet, 0)
    for dy in range(1, Y):
        pl.semaphore_signal(
            barrier, inc=1, device_id=(me, ((y + dy) % Y) * 2 + c), device_id_type=MESH
        )
    pl.semaphore_signal(barrier, inc=1, device_id=(me, sib), device_id_type=MESH)
    pl.semaphore_wait(barrier, (E - 1) + (Y - 1) + 1)

    def rows_of(s):
        return pl.ds(pl.multiple_of(s * C, 16), C)

    def cols_of(t):
        return pl.ds(pl.multiple_of(t * F, 128), F)

    def lanes_of(s):
        return pl.ds(pl.multiple_of(s * N, 128), N)

    def remote(src, dst, ss, rs, dev):
        return pltpu.make_async_remote_copy(
            src_ref=src,
            dst_ref=dst,
            send_sem=ss,
            recv_sem=rs,
            device_id=dev,
            device_id_type=MESH,
        )

    def meta_copy(dst):
        return remote(
            meta_ref.at[dst], meta_out.at[me], meta_send.at[dst], meta_recv.at[me], (dst, tp)
        )

    def tok_copy(dst):
        return remote(
            tok_ref.at[dst],
            xfull.at[rows_of(me), cols_of(tp)],
            tok_send.at[dst],
            tok_recv.at[me],
            (dst, tp),
        )

    def sh_copy(dst):
        return remote(
            sh_ref.at[dst], sh_out.at[:, lanes_of(me)], sh_send.at[dst], sh_recv.at[me], (dst, tp)
        )

    def cot_copy(s, sems, dst):
        return remote(cot_all.at[s], cot_all.at[s], sems.at[s], cot_recv.at[s], (dst, tp))

    locals_ = (
        pltpu.make_async_copy(cot_ref, cot_all.at[me], local_sem.at[0]),
        pltpu.make_async_copy(
            tok_ref.at[me], xfull.at[rows_of(me), cols_of(tp)], local_sem.at[1]
        ),
        pltpu.make_async_copy(meta_ref.at[me], meta_out.at[me], local_sem.at[2]),
        pltpu.make_async_copy(sh_ref.at[me], sh_out.at[:, lanes_of(me)], local_sem.at[3]),
    )
    for cp in locals_:
        cp.start()
    for cp in locals_:
        cp.wait()

    def each_source(fn, first=0):
        def step(i, _):
            k = i // X
            dz = ((k + 1) // 2) * (1 - 2 * (k % 2))
            zs = z + dz
            dx = i % X

            @pl.when((zs >= 0) & (zs < NZ))
            def _():
                fn(i, dz, dx, zs * X + (x + dx) % X)

            return 0

        lax.fori_loop(first, (2 * NZ - 1) * X, step, 0)

    def spread_cot(dz, s, act):
        @pl.when((dz <= 0) & (z + 1 < NZ))
        def _():
            act(cot_copy(s, cot_up, me + X))

        @pl.when((dz >= 0) & (z >= 1))
        def _():
            act(cot_copy(s, cot_down, me - X))

        for d in range(1, X):
            act(cot_copy(s, cot_side.at[d - 1], z * X + (x + d) % X))

    def start(cp):
        cp.start()

    def wait_send(cp):
        cp.wait_send()

    spread_cot(me * 0, me, start)

    def send_small(i, dz, dx, s):
        meta_copy(s).start()

    def send_rows(i, dz, dx, s):
        tok_copy(s).start()

    each_source(send_small, 1)
    each_source(send_rows, 1)

    def y_copy(a, s, dy):
        part = full[a].at[rows_of(s), cols_of(tp)]
        return remote(
            part,
            part,
            y_send.at[a, dy - 1],
            y_recv.at[a, dy - 1, s],
            (me, ((y + dy) % Y) * 2 + c),
        )

    def sib_copy(a, s, dy):
        part = full[a].at[rows_of(s), cols_of(((y + Y - dy) % Y) * 2 + c)]
        return remote(part, part, sib_send.at[a, dy], sib_recv.at[a, dy], (me, sib))

    def forward(a, s):
        for dy in range(1, Y):
            y_copy(a, s, dy).start()
        sib_copy(a, s, 0).start()

    def take_rows(i, dz, dx, s):
        @pl.when(s != me)
        def _():
            remote(
                tok_ref.at[s],
                xfull.at[rows_of(s), cols_of(tp)],
                tok_send.at[s],
                tok_recv.at[s],
                (me, tp),
            ).wait_recv()

        forward(0, s)

    def take_cot(i, dz, dx, s):
        @pl.when(s != me)
        def _():
            remote(
                cot_all.at[s], cot_all.at[s], cot_up.at[s], cot_recv.at[s], (me, tp)
            ).wait_recv()

            @pl.when(dx == 0)
            def _():
                spread_cot(dz, s, start)

            remote(
                meta_ref.at[s], meta_out.at[s], meta_send.at[s], meta_recv.at[s], (me, tp)
            ).wait_recv()

        picked = jnp.dot(
            meta_out[s, :, :N], cot_all[s], preferred_element_type=F32
        ).astype(BF16)
        gfull[rows_of(s), cols_of(tp)] = picked
        forward(1, s)

        @pl.when(s != me)
        def _():
            sh_copy(s).start()

    def relay(a, s):
        for dy in range(1, Y):
            part = full[a].at[rows_of(s), cols_of(((y + Y - dy) % Y) * 2 + c)]
            remote(
                part, part, y_send.at[a, dy - 1], y_recv.at[a, dy - 1, s], (me, tp)
            ).wait_recv()
            sib_copy(a, s, dy).start()

    def relay_rows(i, dz, dx, s):
        relay(0, s)

    def relay_cot(i, dz, dx, s):
        relay(1, s)

    def guarded(fn, j):
        k = j // X
        dz = ((k + 1) // 2) * (1 - 2 * (k % 2))
        zs = z + dz
        dx = j % X

        @pl.when((j >= 0) & (zs >= 0) & (zs < NZ))
        def _():
            fn(j, dz, dx, zs * X + (x + dx) % X)

    total = (2 * NZ - 1) * X

    def main(i, _):
        guarded(take_rows, i)
        guarded(take_cot, i - X)
        guarded(relay_rows, i - X)
        guarded(relay_cot, i - 2 * X)
        return 0

    lax.fori_loop(0, total + 2 * X, main, 0)

    def finish(i, dz, dx, s):
        @pl.when(s != me)
        def _():
            meta_copy(s).wait_send()
            tok_copy(s).wait_send()
            sh_copy(s).wait_send()
            remote(
                sh_ref.at[s], sh_out.at[:, lanes_of(s)], sh_send.at[s], sh_recv.at[s], (me, tp)
            ).wait_recv()

        @pl.when(dx == 0)
        def _():
            spread_cot(dz, s, wait_send)

    each_source(finish)
    for a in (0, 1):
        mine = full[a].at[:, cols_of(tp)]
        for dy in range(1, Y):
            remote(mine, mine, y_send.at[a, dy - 1], y_send.at[a, dy - 1], (me, sib)).wait_send()
        for dy in range(Y):
            other = full[a].at[:, cols_of(((y + Y - dy) % Y) * 2 + 1 - c)]
            cp = remote(other, other, sib_send.at[a, dy], sib_recv.at[a, dy], (me, sib))
            cp.wait_send()
            cp.wait_recv()


def dispatch(E, T, C, F, N, rows, meta, cotangent, shared):
    X = 2 if E % 2 == 0 else 1
    Y = T // 2
    S = shared.shape[1]
    M = meta.shape[2]
    dma = pltpu.SemaphoreType.DMA
    vmem = pl.BlockSpec(memory_space=pltpu.VMEM)
    return pl.pallas_call(
        functools.partial(dispatch_kernel, (E, T, X, C, F, N)),
        out_shape=(
            jax.ShapeDtypeStruct((E * C, T * F), BF16),
            jax.ShapeDtypeStruct((E * C, T * F), BF16),
            jax.ShapeDtypeStruct((E, C, M), BF16),
            jax.ShapeDtypeStruct((E, N, F), BF16),
            jax.ShapeDtypeStruct((S, E * N), BF16),
        ),
        in_specs=[vmem] * 4,
        out_specs=(vmem,) * 5,
        scratch_shapes=[
            dma((4,)),
            dma((E,)),
            dma((E,)),
            dma((E,)),
            dma((E,)),
            dma((E,)),
            dma((E,)),
            dma((E,)),
            dma((E,)),
            dma((max(X - 1, 1), E)),
            dma((E,)),
            dma((2, max(Y - 1, 1))),
            dma((2, max(Y - 1, 1), E)),
            dma((2, Y)),
            dma((2, Y)),
        ],
        compiler_params=pltpu.CompilerParams(
            collective_id=0, has_side_effects=True, vmem_limit_bytes=48 * 1024 * 1024
        ),
        name="dispatch",
    )(rows, meta, cotangent, shared)


def return_kernel(
    dims,
    part,
    gate,
    back,
    gate_back,
    pair_in,
    y_out,
    y_in,
    row_out,
    gate_in,
    gate_out,
    pair_send,
    pair_recv,
    y_send,
    y_recv,
    back_send,
    back_recv,
    gate_tp_send,
    gate_tp_recv,
    gate_ep_send,
    gate_ep_recv,
):
    E, T, C, F = dims
    Y = T // 2
    me = lax.axis_index("ep")
    tp = lax.axis_index("tp")
    y = tp // 2
    c = tp % 2
    sib = y * 2 + (1 - c)

    barrier = pltpu.get_barrier_semaphore()

    def greet(d, _):
        pl.semaphore_signal(
            barrier, inc=1, device_id=((me + d) % E, tp), device_id_type=MESH
        )
        return 0

    lax.fori_loop(1, E, greet, 0)
    for dt in range(1, T):
        pl.semaphore_signal(
            barrier, inc=1, device_id=(me, (tp + dt) % T), device_id_type=MESH
        )
    pl.semaphore_wait(barrier, (E - 1) + (T - 1))

    def rows_of(s):
        return pl.ds(pl.multiple_of(s * C, 16), C)

    def cols_of(t):
        return pl.ds(pl.multiple_of(t * F, 128), F)

    def remote(src, dst, ss, rs, dev):
        return pltpu.make_async_remote_copy(
            src_ref=src,
            dst_ref=dst,
            send_sem=ss,
            recv_sem=rs,
            device_id=dev,
            device_id_type=MESH,
        )

    def source(i):
        return (me + E // 2 + i) % E

    def pair_copy(s, dy):
        return remote(
            part.at[rows_of(s), cols_of(((y + dy) % Y) * 2 + 1 - c)],
            pair_in.at[dy, rows_of(s)],
            pair_send.at[dy],
            pair_recv.at[dy, s],
            (me, sib),
        )

    def gate_tp_copy(dt):
        return remote(
            gate, gate_in.at[dt], gate_tp_send.at[dt], gate_tp_recv.at[dt], (me, (tp + dt) % T)
        )

    def gate_ep_copy(s):
        return remote(gate_out.at[s], gate_back.at[me], gate_ep_send, gate_ep_recv, (s, tp))

    def y_copy(s, dy):
        return remote(
            y_out.at[dy - 1, rows_of(s)],
            y_in.at[dy - 1, rows_of(s)],
            y_send.at[dy - 1],
            y_recv.at[dy - 1, s],
            (me, ((y + dy) % Y) * 2 + c),
        )

    def back_copy(s):
        return remote(row_out.at[rows_of(s)], back.at[me], back_send, back_recv, (s, tp))

    for dt in range(1, T):
        gate_tp_copy(dt).start()

    def open_pairs(i, _):
        for dy in list(range(1, Y)) + [0]:
            pair_copy(source(i), dy).start()
        return 0

    lax.fori_loop(0, E, open_pairs, 0)

    def mix(s, dy):
        pair_copy(s, dy).wait_recv()
        return part[rows_of(s), cols_of(((y + dy) % Y) * 2 + c)].astype(F32) + pair_in[
            dy, rows_of(s), :
        ].astype(F32)

    def cross(s):
        for dy in range(1, Y):
            y_out[dy - 1, rows_of(s), :] = mix(s, dy).astype(BF16)
            y_copy(s, dy).start()

    def send_back(s):
        value = mix(s, 0)
        for dy in range(1, Y):
            y_copy(s, dy).wait_recv()
            value = value + y_in[dy - 1, rows_of(s), :].astype(F32)
        value = value.astype(BF16)

        @pl.when(s != me)
        def _():
            row_out[rows_of(s), :] = value
            back_copy(s).start()

        @pl.when(s == me)
        def _():
            back[me] = value

    def main(i, _):
        @pl.when(i < E)
        def _():
            cross(source(i))

        @pl.when(i >= 2)
        def _():
            send_back(source(i - 2))

        return 0

    lax.fori_loop(0, E + 2, main, 0)

    total = gate[...]
    for dt in range(1, T):
        gate_tp_copy(dt).wait()
        total = total + gate_in[dt]
    gate_out[...] = total
    gate_back[me] = gate_out[me]

    def gates(d, _):
        gate_ep_copy((me + d) % E).start()
        return 0

    lax.fori_loop(1, E, gates, 0)

    for dy in range(Y):
        everything = pair_in.at[dy]
        remote(everything, everything, pair_send.at[dy], pair_send.at[dy], (me, sib)).wait_send()
    for dy in range(1, Y):
        everything = y_in.at[dy - 1]
        remote(everything, everything, y_send.at[dy - 1], y_send.at[dy - 1], (me, sib)).wait_send()
    blocks = back.at[pl.ds(0, E - 1)]
    done = remote(blocks, blocks, back_send, back_recv, (me, sib))
    done.wait_send()
    done.wait_recv()
    blocks = gate_back.at[pl.ds(0, E - 1)]
    done = remote(blocks, blocks, gate_ep_send, gate_ep_recv, (me, sib))
    done.wait_send()
    done.wait_recv()


def send_home(E, T, C, F, part, gate):
    Y = T // 2
    R = E * C
    dma = pltpu.SemaphoreType.DMA
    vmem = pl.BlockSpec(memory_space=pltpu.VMEM)
    return pl.pallas_call(
        functools.partial(return_kernel, (E, T, C, F)),
        out_shape=(
            jax.ShapeDtypeStruct((E, C, F), BF16),
            jax.ShapeDtypeStruct(gate.shape, F32),
        ),
        in_specs=[vmem] * 2,
        out_specs=(vmem,) * 2,
        scratch_shapes=[
            pltpu.VMEM((Y, R, F), BF16),
            pltpu.VMEM((max(Y - 1, 1), R, F), BF16),
            pltpu.VMEM((max(Y - 1, 1), R, F), BF16),
            pltpu.VMEM((R, F), BF16),
            pltpu.VMEM((T,) + gate.shape, F32),
            pltpu.VMEM(gate.shape, F32),
            dma((Y,)),
            dma((Y, E)),
            dma((max(Y - 1, 1),)),
            dma((max(Y - 1, 1), E)),
            dma,
            dma,
            dma((T,)),
            dma((T,)),
            dma,
            dma,
        ],
        compiler_params=pltpu.CompilerParams(
            collective_id=1, has_side_effects=True, vmem_limit_bytes=40 * 1024 * 1024
        ),
        name="send_home",
    )(part, gate)


def shards(tokens, cotangent, routes, gate_weight, w_gate, w_up, w_down, shared_hidden):
    tok_count, top_count = routes.shape
    E = lax.axis_size("ep")
    T = lax.axis_size("tp")
    F = tokens.shape[1]
    capacity = 3 * tok_count * top_count // (2 * E)
    C = -(-capacity // 16) * 16
    R = E * C
    flat_routes = routes.reshape(-1)
    onehot = (flat_routes[:, None] == jnp.arange(E, dtype=jnp.int32)[None, :]).astype(F32)
    count = tok_count * top_count
    before = (
        jnp.arange(count, dtype=jnp.int32)[:, None] > jnp.arange(count, dtype=jnp.int32)[None, :]
    ).astype(BF16)
    earlier = jnp.dot(before, onehot.astype(BF16), preferred_element_type=F32)
    positions = jnp.sum(earlier * onehot, axis=1).astype(jnp.int32)
    slots = (flat_routes * C + positions).reshape(tok_count, top_count)
    lines = jnp.arange(R, dtype=jnp.int32)[:, None]
    masks = [slots[:, k][None, :] == lines for k in range(top_count)]
    select = functools.reduce(jnp.logical_or, masks).astype(BF16)
    weight = sum(
        jnp.sum(jnp.where(m, gate_weight[:, k][None, :], 0.0), axis=1)
        for k, m in enumerate(masks)
    )
    high = lax.reduce_precision(weight, 8, 7)
    low = weight - high
    tail = jnp.arange(128, dtype=jnp.int32)[None, :]
    extra = jnp.where(
        tail == 0, high[:, None], jnp.where(tail == 1, low[:, None], 0.0)
    ).astype(BF16)
    meta = jnp.concatenate([select, extra], axis=1).reshape(E, C, tok_count + 128)
    rows = jnp.dot(select, tokens, preferred_element_type=F32).astype(BF16).reshape(E, C, F)
    shared = shared_hidden.T.reshape(E, shared_hidden.shape[1] // E, tok_count)

    rows_x, rows_g, meta_got, cot_all, shared_got = dispatch(
        E, T, C, F, tok_count, rows, meta, cotangent, shared
    )
    got = meta_got.reshape(R, tok_count + 128)
    weight_col = got[:, tok_count : tok_count + 1].astype(F32) + got[
        :, tok_count + 1 : tok_count + 2
    ].astype(F32)
    contract_last = (((1,), (1,)), ((), ()))
    gate_mat = w_gate[0]
    up_mat = w_up[0]
    down_mat = w_down[0]
    pre_gate = lax.dot_general(rows_x, gate_mat, contract_last, preferred_element_type=F32)
    pre_up = lax.dot_general(rows_x, up_mat, contract_last, preferred_element_type=F32)
    sigmoid_gate = jax.nn.sigmoid(pre_gate)
    silu_gate = pre_gate * sigmoid_gate
    hidden = (silu_gate * pre_up).astype(BF16)
    back_hidden = lax.dot_general(rows_g, down_mat, contract_last, preferred_element_type=F32)
    gate_part = jnp.sum(hidden.astype(F32) * back_hidden, axis=1)
    scaled = weight_col * back_hidden
    grad_pre_gate = (
        scaled * pre_up * sigmoid_gate * (1.0 + pre_gate * (1.0 - sigmoid_gate))
    ).astype(BF16)
    grad_pre_up = (scaled * silu_gate).astype(BF16)
    weighted_cotan = (weight_col * rows_g.astype(F32)).astype(BF16)
    grad_down = jnp.dot(hidden.T, weighted_cotan, preferred_element_type=F32)
    grad_gate = jnp.dot(grad_pre_gate.T, rows_x, preferred_element_type=F32)
    grad_up = jnp.dot(grad_pre_up.T, rows_x, preferred_element_type=F32)
    partial_value = jnp.dot(grad_pre_gate, gate_mat, preferred_element_type=F32)
    partial_value = partial_value + jnp.dot(grad_pre_up, up_mat, preferred_element_type=F32)
    shared_grad = jnp.dot(
        shared_got, cot_all.reshape(E * tok_count, F), preferred_element_type=F32
    )
    gate_box = jnp.pad(gate_part.reshape(E, 1, C), ((0, 0), (0, 7), (0, 128 - C)))
    back_rows, back_gate = send_home(E, T, C, F, partial_value.astype(BF16), gate_box)
    back_gate = back_gate[:, 0, :C]
    tokens_grad = lax.dot_general(
        select, back_rows.reshape(R, F), (((0,), (0,)), ((), ())), preferred_element_type=F32
    ).astype(BF16)
    gate_grad = jnp.stack(
        [jnp.sum(jnp.where(m, back_gate.reshape(R, 1), 0.0), axis=0) for m in masks], axis=1
    )
    return (tokens_grad, gate_grad, grad_gate[None], grad_up[None], grad_down[None], shared_grad)


def solution(mesh):
    placed = (
        P("ep", "tp"),
        P("ep", "tp"),
        P("ep", None),
        P("ep", None),
        P("ep", "tp", None),
        P("ep", "tp", None),
        P("ep", "tp", None),
        P("ep", None),
    )
    return jax.shard_map(
        shards,
        mesh=mesh,
        in_specs=placed,
        out_specs=(
            P("ep", "tp"),
            P("ep", None),
            P("ep", "tp", None),
            P("ep", "tp", None),
            P("ep", "tp", None),
            P("ep", "tp"),
        ),
        check_vma=False,
    )
```

```python
import functools

import jax
import jax.numpy as jnp
from jax import lax
from jax.experimental import pallas as pl
from jax.experimental.pallas import tpu as pltpu
from jax.sharding import PartitionSpec as P

MESH = pl.DeviceIdType.MESH
BF16 = jnp.bfloat16
F32 = jnp.float32


def dispatch_kernel(
    dims,
    tok_ref,
    meta_ref,
    cot_ref,
    sh_ref,
    xfull,
    gfull,
    meta_out,
    cot_all,
    sh_out,
    local_sem,
    meta_send,
    meta_recv,
    tok_send,
    tok_recv,
    sh_send,
    sh_recv,
    cot_up,
    cot_down,
    cot_side,
    cot_recv,
    y_send,
    y_recv,
    sib_send,
    sib_recv,
):
    E, T, X, C, F, N = dims
    Y = T // 2
    NZ = E // X
    me = lax.axis_index("ep")
    tp = lax.axis_index("tp")
    y = tp // 2
    c = tp % 2
    sib = y * 2 + (1 - c)
    z = me // X
    x = me % X
    full = (xfull, gfull)

    barrier = pltpu.get_barrier_semaphore()

    def greet(d, _):
        pl.semaphore_signal(
            barrier, inc=1, device_id=((me + d) % E, tp), device_id_type=MESH
        )
        return 0

    lax.fori_loop(1, E, greet, 0)
    for dt in range(1, T):
        pl.semaphore_signal(
            barrier, inc=1, device_id=(me, (tp + dt) % T), device_id_type=MESH
        )
    pl.semaphore_wait(barrier, (E - 1) + (T - 1))

    def rows_of(s):
        return pl.ds(pl.multiple_of(s * C, 16), C)

    def cols_of(t):
        return pl.ds(pl.multiple_of(t * F, 128), F)

    def lanes_of(s):
        return pl.ds(pl.multiple_of(s * N, 128), N)

    def remote(src, dst, ss, rs, dev):
        return pltpu.make_async_remote_copy(
            src_ref=src,
            dst_ref=dst,
            send_sem=ss,
            recv_sem=rs,
            device_id=dev,
            device_id_type=MESH,
        )

    def meta_copy(dst):
        return remote(
            meta_ref.at[dst], meta_out.at[me], meta_send.at[dst], meta_recv.at[me], (dst, tp)
        )

    def tok_copy(dst):
        return remote(
            tok_ref.at[dst],
            xfull.at[rows_of(me), cols_of(tp)],
            tok_send.at[dst],
            tok_recv.at[me],
            (dst, tp),
        )

    def sh_copy(dst):
        return remote(
            sh_ref.at[dst], sh_out.at[:, lanes_of(me)], sh_send.at[dst], sh_recv.at[me], (dst, tp)
        )

    def cot_copy(s, sems, dst):
        return remote(cot_all.at[s], cot_all.at[s], sems.at[s], cot_recv.at[s], (dst, tp))

    locals_ = (
        pltpu.make_async_copy(cot_ref, cot_all.at[me], local_sem.at[0]),
        pltpu.make_async_copy(
            tok_ref.at[me], xfull.at[rows_of(me), cols_of(tp)], local_sem.at[1]
        ),
        pltpu.make_async_copy(meta_ref.at[me], meta_out.at[me], local_sem.at[2]),
        pltpu.make_async_copy(sh_ref.at[me], sh_out.at[:, lanes_of(me)], local_sem.at[3]),
    )
    for cp in locals_:
        cp.start()
    for cp in locals_:
        cp.wait()

    def each_source(fn, first=0):
        def step(i, _):
            k = i // X
            dz = ((k + 1) // 2) * (1 - 2 * (k % 2))
            zs = z + dz
            dx = i % X

            @pl.when((zs >= 0) & (zs < NZ))
            def _():
                fn(i, dz, dx, zs * X + (x + dx) % X)

            return 0

        lax.fori_loop(first, (2 * NZ - 1) * X, step, 0)

    def spread_cot(dz, s, act):
        @pl.when((dz <= 0) & (z + 1 < NZ))
        def _():
            act(cot_copy(s, cot_up, me + X))

        @pl.when((dz >= 0) & (z >= 1))
        def _():
            act(cot_copy(s, cot_down, me - X))

        for d in range(1, X):
            act(cot_copy(s, cot_side.at[d - 1], z * X + (x + d) % X))

    def start(cp):
        cp.start()

    def wait_send(cp):
        cp.wait_send()

    spread_cot(me * 0, me, start)

    def send_small(i, dz, dx, s):
        meta_copy(s).start()

    def send_rows(i, dz, dx, s):
        tok_copy(s).start()

    each_source(send_small, 1)
    each_source(send_rows, 1)

    def y_copy(a, s, dy):
        part = full[a].at[rows_of(s), cols_of(tp)]
        return remote(
            part,
            part,
            y_send.at[a, dy - 1],
            y_recv.at[a, dy - 1, s],
            (me, ((y + dy) % Y) * 2 + c),
        )

    def sib_copy(a, s, dy):
        part = full[a].at[rows_of(s), cols_of(((y + Y - dy) % Y) * 2 + c)]
        return remote(part, part, sib_send.at[a, dy], sib_recv.at[a, dy], (me, sib))

    def forward(a, s):
        for dy in range(1, Y):
            y_copy(a, s, dy).start()
        sib_copy(a, s, 0).start()

    def take_rows(i, dz, dx, s):
        @pl.when(s != me)
        def _():
            remote(
                tok_ref.at[s],
                xfull.at[rows_of(s), cols_of(tp)],
                tok_send.at[s],
                tok_recv.at[s],
                (me, tp),
            ).wait_recv()

        forward(0, s)

    def take_cot(i, dz, dx, s):
        @pl.when(s != me)
        def _():
            remote(
                cot_all.at[s], cot_all.at[s], cot_up.at[s], cot_recv.at[s], (me, tp)
            ).wait_recv()

            @pl.when(dx == 0)
            def _():
                spread_cot(dz, s, start)

            remote(
                meta_ref.at[s], meta_out.at[s], meta_send.at[s], meta_recv.at[s], (me, tp)
            ).wait_recv()

        picked = jnp.dot(
            meta_out[s, :, :N], cot_all[s], preferred_element_type=F32
        ).astype(BF16)
        gfull[rows_of(s), cols_of(tp)] = picked
        forward(1, s)

        @pl.when(s != me)
        def _():
            sh_copy(s).start()

    def relay(a, s):
        for dy in range(1, Y):
            part = full[a].at[rows_of(s), cols_of(((y + Y - dy) % Y) * 2 + c)]
            remote(
                part, part, y_send.at[a, dy - 1], y_recv.at[a, dy - 1, s], (me, tp)
            ).wait_recv()
            sib_copy(a, s, dy).start()

    def relay_rows(i, dz, dx, s):
        relay(0, s)

    def relay_cot(i, dz, dx, s):
        relay(1, s)

    def guarded(fn, j):
        k = j // X
        dz = ((k + 1) // 2) * (1 - 2 * (k % 2))
        zs = z + dz
        dx = j % X

        @pl.when((j >= 0) & (zs >= 0) & (zs < NZ))
        def _():
            fn(j, dz, dx, zs * X + (x + dx) % X)

    total = (2 * NZ - 1) * X

    def main(i, _):
        guarded(take_rows, i)
        guarded(take_cot, i - X)
        guarded(relay_rows, i - X)
        guarded(relay_cot, i - 2 * X)
        return 0

    lax.fori_loop(0, total + 2 * X, main, 0)

    def finish(i, dz, dx, s):
        @pl.when(s != me)
        def _():
            meta_copy(s).wait_send()
            tok_copy(s).wait_send()
            sh_copy(s).wait_send()
            remote(
                sh_ref.at[s], sh_out.at[:, lanes_of(s)], sh_send.at[s], sh_recv.at[s], (me, tp)
            ).wait_recv()

        @pl.when(dx == 0)
        def _():
            spread_cot(dz, s, wait_send)

    each_source(finish)
    for a in (0, 1):
        mine = full[a].at[:, cols_of(tp)]
        for dy in range(1, Y):
            remote(mine, mine, y_send.at[a, dy - 1], y_send.at[a, dy - 1], (me, sib)).wait_send()
        for dy in range(Y):
            other = full[a].at[:, cols_of(((y + Y - dy) % Y) * 2 + 1 - c)]
            cp = remote(other, other, sib_send.at[a, dy], sib_recv.at[a, dy], (me, sib))
            cp.wait_send()
            cp.wait_recv()


def return_kernel(
    dims,
    part,
    gate,
    back,
    gate_back,
    pair_in,
    y_out,
    y_in,
    row_out,
    gate_in,
    gate_out,
    pair_send,
    pair_recv,
    y_send,
    y_recv,
    back_send,
    back_recv,
    gate_tp_send,
    gate_tp_recv,
    gate_ep_send,
    gate_ep_recv,
):
    E, T, C, F = dims
    Y = T // 2
    me = lax.axis_index("ep")
    tp = lax.axis_index("tp")
    y = tp // 2
    c = tp % 2
    sib = y * 2 + (1 - c)

    def rows_of(s):
        return pl.ds(pl.multiple_of(s * C, 16), C)

    def cols_of(t):
        return pl.ds(pl.multiple_of(t * F, 128), F)

    def remote(src, dst, ss, rs, dev):
        return pltpu.make_async_remote_copy(
            src_ref=src,
            dst_ref=dst,
            send_sem=ss,
            recv_sem=rs,
            device_id=dev,
            device_id_type=MESH,
        )

    def source(i):
        return (me + E // 2 + i) % E

    def pair_copy(s, dy):
        return remote(
            part.at[rows_of(s), cols_of(((y + dy) % Y) * 2 + 1 - c)],
            pair_in.at[dy, rows_of(s)],
            pair_send.at[dy],
            pair_recv.at[dy, s],
            (me, sib),
        )

    def gate_tp_copy(dt):
        return remote(
            gate, gate_in.at[dt], gate_tp_send.at[dt], gate_tp_recv.at[dt], (me, (tp + dt) % T)
        )

    def gate_ep_copy(s):
        return remote(gate_out.at[s], gate_back.at[me], gate_ep_send, gate_ep_recv, (s, tp))

    def y_copy(s, dy):
        return remote(
            y_out.at[dy - 1, rows_of(s)],
            y_in.at[dy - 1, rows_of(s)],
            y_send.at[dy - 1],
            y_recv.at[dy - 1, s],
            (me, ((y + dy) % Y) * 2 + c),
        )

    def back_copy(s):
        return remote(row_out.at[rows_of(s)], back.at[me], back_send, back_recv, (s, tp))

    for dt in range(1, T):
        gate_tp_copy(dt).start()

    def open_pairs(i, _):
        for dy in list(range(1, Y)) + [0]:
            pair_copy(source(i), dy).start()
        return 0

    lax.fori_loop(0, E, open_pairs, 0)

    def mix(s, dy):
        pair_copy(s, dy).wait_recv()
        return part[rows_of(s), cols_of(((y + dy) % Y) * 2 + c)].astype(F32) + pair_in[
            dy, rows_of(s), :
        ].astype(F32)

    def cross(s):
        for dy in range(1, Y):
            y_out[dy - 1, rows_of(s), :] = mix(s, dy).astype(BF16)
            y_copy(s, dy).start()

    def send_back(s):
        value = mix(s, 0)
        for dy in range(1, Y):
            y_copy(s, dy).wait_recv()
            value = value + y_in[dy - 1, rows_of(s), :].astype(F32)
        value = value.astype(BF16)

        @pl.when(s != me)
        def _():
            row_out[rows_of(s), :] = value
            back_copy(s).start()

        @pl.when(s == me)
        def _():
            back[me] = value

    def main(i, _):
        @pl.when(i < E)
        def _():
            cross(source(i))

        @pl.when(i >= 2)
        def _():
            send_back(source(i - 2))

        return 0

    lax.fori_loop(0, E + 2, main, 0)

    total = gate[...]
    for dt in range(1, T):
        gate_tp_copy(dt).wait()
        total = total + gate_in[dt]
    gate_out[...] = total
    gate_back[me] = gate_out[me]

    def gates(d, _):
        gate_ep_copy((me + d) % E).start()
        return 0

    lax.fori_loop(1, E, gates, 0)

    for dy in range(Y):
        everything = pair_in.at[dy]
        remote(everything, everything, pair_send.at[dy], pair_send.at[dy], (me, sib)).wait_send()
    for dy in range(1, Y):
        everything = y_in.at[dy - 1]
        remote(everything, everything, y_send.at[dy - 1], y_send.at[dy - 1], (me, sib)).wait_send()
    blocks = back.at[pl.ds(0, E - 1)]
    done = remote(blocks, blocks, back_send, back_recv, (me, sib))
    done.wait_send()
    done.wait_recv()
    blocks = gate_back.at[pl.ds(0, E - 1)]
    done = remote(blocks, blocks, gate_ep_send, gate_ep_recv, (me, sib))
    done.wait_send()
    done.wait_recv()


def expert_compute(
    dims, xfull, gfull, meta_out, hidden, grad_gate, grad_up, wg, wu, wd, accs, part, gate
):
    E, T, C, F, N = dims
    acc_g, acc_u, acc_b = accs.at[0], accs.at[1], accs.at[2]
    nt = (((1,), (1,)), ((), ()))
    accs[...] = jnp.zeros_like(accs)

    def forward(t, _):
        cols = pl.ds(pl.multiple_of(t * F, 128), F)
        acc_g[...] += lax.dot_general(
            xfull[:, cols], wg[:, cols], nt, preferred_element_type=F32
        )
        acc_u[...] += lax.dot_general(
            xfull[:, cols], wu[:, cols], nt, preferred_element_type=F32
        )
        acc_b[...] += lax.dot_general(
            gfull[:, cols], wd[:, cols], nt, preferred_element_type=F32
        )
        return 0

    lax.fori_loop(0, T, forward, 0)
    diagonal = lax.broadcasted_iota(jnp.int32, (C, 128), 0) == lax.broadcasted_iota(
        jnp.int32, (C, 128), 1
    )

    def middle(s, _):
        rows = pl.ds(pl.multiple_of(s * C, 16), C)
        pre_gate = acc_g[rows, :]
        pre_up = acc_u[rows, :]
        back = acc_b[rows, :]
        weight = meta_out[s, :, N : N + 128].astype(F32)
        weight = weight[:, 0:1] + weight[:, 1:2]
        sigmoid_gate = jax.nn.sigmoid(pre_gate)
        silu_gate = pre_gate * sigmoid_gate
        hid = (silu_gate * pre_up).astype(BF16)
        hidden[rows, :] = hid
        column = jnp.sum(hid.astype(F32) * back, axis=1, keepdims=True)
        line = jnp.sum(jnp.where(diagonal, column, 0.0), axis=0, keepdims=True)
        gate[s] = jnp.broadcast_to(line, (8, 128))
        scaled = weight * back
        grad_gate[rows, :] = (
            scaled * pre_up * sigmoid_gate * (1.0 + pre_gate * (1.0 - sigmoid_gate))
        ).astype(BF16)
        grad_up[rows, :] = (scaled * silu_gate).astype(BF16)
        return 0

    lax.fori_loop(0, E, middle, 0)

    def partial(t, _):
        cols = pl.ds(pl.multiple_of(t * F, 128), F)
        part[:, cols] = (
            jnp.dot(grad_gate[...], wg[:, cols], preferred_element_type=F32)
            + jnp.dot(grad_up[...], wu[:, cols], preferred_element_type=F32)
        ).astype(BF16)
        return 0

    lax.fori_loop(0, T, partial, 0)


def whole_kernel(dims, n_dispatch, *refs):
    E, T, X, C, F, N = dims
    tok, meta, cot, sh, w_gate, w_up, w_down = refs[:7]
    xfull, gfull, meta_out, cot_all, sh_out, hidden, grad_gate, grad_up, back, gate_back = refs[
        7:17
    ]
    wg, wu, wd, accs, part, gate, load_sem = refs[17:24]
    rest = refs[24:]
    loads = [
        pltpu.make_async_copy(src.at[0], dst, load_sem.at[i])
        for i, (src, dst) in enumerate(((w_gate, wg), (w_up, wu), (w_down, wd)))
    ]
    for cp in loads:
        cp.start()
    dispatch_kernel(
        dims,
        tok,
        meta,
        cot,
        sh,
        xfull,
        gfull,
        meta_out,
        cot_all,
        sh_out,
        *rest[:n_dispatch],
    )
    for cp in loads:
        cp.wait()
    expert_compute(
        (E, T, C, F, N),
        xfull,
        gfull,
        meta_out,
        hidden,
        grad_gate,
        grad_up,
        wg,
        wu,
        wd,
        accs,
        part,
        gate,
    )
    return_kernel((E, T, C, F), part, gate, back, gate_back, *rest[n_dispatch:])


def routed(E, T, C, F, N, rows, meta, cotangent, shared, w_gate, w_up, w_down):
    X = 2 if E % 2 == 0 else 1
    Y = T // 2
    Z = max(Y - 1, 1)
    R = E * C
    S = shared.shape[1]
    H = w_gate.shape[1]
    dma = pltpu.SemaphoreType.DMA
    vmem = pl.BlockSpec(memory_space=pltpu.VMEM)
    anywhere = pl.BlockSpec(memory_space=pl.ANY)
    shape = jax.ShapeDtypeStruct
    sems = [
        dma((4,)),
        dma((E,)),
        dma((E,)),
        dma((E,)),
        dma((E,)),
        dma((E,)),
        dma((E,)),
        dma((E,)),
        dma((E,)),
        dma((max(X - 1, 1), E)),
        dma((E,)),
        dma((2, Z)),
        dma((2, Z, E)),
        dma((2, Y)),
        dma((2, Y)),
    ]
    home = [
        pltpu.VMEM((Y, R, F), BF16),
        pltpu.VMEM((Z, R, F), BF16),
        pltpu.VMEM((Z, R, F), BF16),
        pltpu.VMEM((R, F), BF16),
        pltpu.VMEM((T, E, 8, 128), F32),
        pltpu.VMEM((E, 8, 128), F32),
        dma((Y,)),
        dma((Y, E)),
        dma((Z,)),
        dma((Z, E)),
        dma,
        dma,
        dma((T,)),
        dma((T,)),
        dma,
        dma,
    ]
    return pl.pallas_call(
        functools.partial(whole_kernel, (E, T, X, C, F, N), len(sems)),
        out_shape=(
            shape((R, T * F), BF16),
            shape((R, T * F), BF16),
            shape(meta.shape, BF16),
            shape((E, N, F), BF16),
            shape((S, E * N), BF16),
            shape((R, H), BF16),
            shape((R, H), BF16),
            shape((R, H), BF16),
            shape((E, C, F), BF16),
            shape((E, 8, 128), F32),
        ),
        in_specs=[vmem] * 4 + [anywhere] * 3,
        out_specs=(vmem,) * 10,
        scratch_shapes=[
            pltpu.VMEM((H, T * F), BF16),
            pltpu.VMEM((H, T * F), BF16),
            pltpu.VMEM((H, T * F), BF16),
            pltpu.VMEM((3, R, H), F32),
            pltpu.VMEM((R, T * F), BF16),
            pltpu.VMEM((E, 8, 128), F32),
            dma((3,)),
        ]
        + sems
        + home,
        compiler_params=pltpu.CompilerParams(
            collective_id=0, has_side_effects=True, vmem_limit_bytes=56 * 1024 * 1024
        ),
        name="routed",
    )(rows, meta, cotangent, shared, w_gate, w_up, w_down)


def shards(tokens, cotangent, routes, gate_weight, w_gate, w_up, w_down, shared_hidden):
    tok_count, top_count = routes.shape
    E = lax.axis_size("ep")
    T = lax.axis_size("tp")
    F = tokens.shape[1]
    capacity = 3 * tok_count * top_count // (2 * E)
    C = -(-capacity // 16) * 16
    R = E * C
    flat_routes = routes.reshape(-1)
    onehot = (flat_routes[:, None] == jnp.arange(E, dtype=jnp.int32)[None, :]).astype(F32)
    count = tok_count * top_count
    before = (
        jnp.arange(count, dtype=jnp.int32)[:, None] > jnp.arange(count, dtype=jnp.int32)[None, :]
    ).astype(BF16)
    earlier = jnp.dot(before, onehot.astype(BF16), preferred_element_type=F32)
    positions = jnp.sum(earlier * onehot, axis=1).astype(jnp.int32)
    slots = (flat_routes * C + positions).reshape(tok_count, top_count)
    lines = jnp.arange(R, dtype=jnp.int32)[:, None]
    masks = [slots[:, k][None, :] == lines for k in range(top_count)]
    select = functools.reduce(jnp.logical_or, masks).astype(BF16)
    weight = sum(
        jnp.sum(jnp.where(m, gate_weight[:, k][None, :], 0.0), axis=1)
        for k, m in enumerate(masks)
    )
    high = lax.reduce_precision(weight, 8, 7)
    low = weight - high
    tail = jnp.arange(128, dtype=jnp.int32)[None, :]
    extra = jnp.where(
        tail == 0, high[:, None], jnp.where(tail == 1, low[:, None], 0.0)
    ).astype(BF16)
    meta = jnp.concatenate([select, extra], axis=1).reshape(E, C, tok_count + 128)
    rows = jnp.dot(select, tokens, preferred_element_type=F32).astype(BF16).reshape(E, C, F)
    shared = shared_hidden.T.reshape(E, shared_hidden.shape[1] // E, tok_count)

    (
        rows_x,
        rows_g,
        meta_got,
        cot_all,
        shared_got,
        hidden,
        grad_pre_gate,
        grad_pre_up,
        back_rows,
        back_gate,
    ) = routed(
        E, T, C, F, tok_count, rows, meta, cotangent, shared, w_gate, w_up, w_down
    )
    got = meta_got.reshape(R, tok_count + 128)
    weight_col = got[:, tok_count : tok_count + 1].astype(F32) + got[
        :, tok_count + 1 : tok_count + 2
    ].astype(F32)
    weighted_cotan = (weight_col * rows_g.astype(F32)).astype(BF16)
    grad_down = jnp.dot(hidden.T, weighted_cotan, preferred_element_type=F32)
    grad_gate = jnp.dot(grad_pre_gate.T, rows_x, preferred_element_type=F32)
    grad_up = jnp.dot(grad_pre_up.T, rows_x, preferred_element_type=F32)
    shared_grad = jnp.dot(
        shared_got, cot_all.reshape(E * tok_count, F), preferred_element_type=F32
    )
    back_gate = back_gate[:, 0, :C]
    tokens_grad = lax.dot_general(
        select, back_rows.reshape(R, F), (((0,), (0,)), ((), ())), preferred_element_type=F32
    ).astype(BF16)
    gate_grad = jnp.stack(
        [jnp.sum(jnp.where(m, back_gate.reshape(R, 1), 0.0), axis=0) for m in masks], axis=1
    )
    return (tokens_grad, gate_grad, grad_gate[None], grad_up[None], grad_down[None], shared_grad)


def solution(mesh):
    placed = (
        P("ep", "tp"),
        P("ep", "tp"),
        P("ep", None),
        P("ep", None),
        P("ep", "tp", None),
        P("ep", "tp", None),
        P("ep", "tp", None),
        P("ep", None),
    )
    return jax.shard_map(
        shards,
        mesh=mesh,
        in_specs=placed,
        out_specs=(
            P("ep", "tp"),
            P("ep", None),
            P("ep", "tp", None),
            P("ep", "tp", None),
            P("ep", "tp", None),
            P("ep", "tp"),
        ),
        check_vma=False,
    )
```
